32 devices in a mesh: ep: 16 (over z, y, x), tp: 2 (over core).
Axes of the slice: x: 2, y: 2, z: 4, core: 2. Of those that a mesh axis runs over, the one named last changes fastest.
Arguments:
- tokens: bfloat16 [512, 1024], P('ep'), may hold values from -6 to 6
- norm_gain: float32 [1024], replicated, may hold values from 0.1 to 1.9
- routing: int32 [512, 4], P('ep'), may hold values from 0 to 15, all different within a row; in each aligned block of 32 rows (0 to 31, 32 to 63, ...) at most 16 rows name the same one
- route_logits: float32 [512, 4], P('ep'), may hold values from -6 to 6
- w_gate: bfloat16 [16, 1024, 1024], P('ep', None, 'tp'), may hold values from -0.1875 to 0.1875
- w_up: bfloat16 [16, 1024, 1024], P('ep', None, 'tp'), may hold values from -0.1875 to 0.1875
- w_down: bfloat16 [16, 1024, 1024], P('ep', None, 'tp'), may hold values from -0.1875 to 0.1875
Outputs:
- mixed: bfloat16 [512, 1024], P('ep', 'tp')
The draws below stay inside these ranges and needn't reach their ends.
Inputs may be any that keep to these rules, and one draw needn't show every extreme that they name: `routing`: each row names 4 different experts; among the 32 tokens of one index of ep (aligned blocks of rows) no expert is named by more than 16 rows, and some block has an expert named by exactly 16.
All inputs are finite; a program needn't handle non-finite values.
Results may differ from the reference program's by a relative error of at most 0.0085.
Values may be sent and summed in bfloat16 or wider, within the bound.
A program may use at most 64 MiB of HBM per device.

```python
import math
import jax
import jax.numpy as jnp
import numpy as np
from jax import lax

D = 1024
FF = 1024
TOPK = 4
TOK_DEV = 32
TOKENS = 512
EXPERTS = 16
CAP = 16


def block_levels(stream_key, dims, shards, smallest, largest):
    def one(axis_at, parts):
        steps = jax.random.uniform(jax.random.fold_in(jax.random.fold_in(stream_key, 6), axis_at), (parts,), jnp.float32, smallest / len(shards), largest / len(shards))
        return jnp.repeat(jnp.exp(steps), dims[axis_at] // parts).reshape((-1,) + (1,) * (len(dims) - axis_at - 1))

    level = one(*shards[0])
    for cut in shards[1:]:
        level = level * one(*cut)
    return level


def routed_block(stream_key, own, number, rows, count, top, reach, skew):
    ranking = jax.random.permutation(stream_key, count)
    packed, ordinary = portions_of(count, rows * top, reach, skew, True), portions_of(count, rows * top, reach, skew, False)
    places = jnp.arange(count)

    def named(tallies, rotation):
        used = int((tallies > 0).sum())
        fixed = max(1, used // 4)
        passed = fixed + (places - fixed + rotation * (used - fixed)) % max(1, count - fixed)
        return jnp.zeros((count,), jnp.int32).at[ranking[jnp.where(places < fixed, places, passed)]].set(jnp.asarray(tallies, jnp.int32))

    tallies = jnp.where(number % 4 == 0, named(packed, number // 4), named(ordinary, number - number // 4 - 1))
    mixed = jax.random.permutation(jax.random.fold_in(own, 3), count)
    donor, taker = mixed[0:count // 2 * 2:2], mixed[1:count // 2 * 2:2]
    slack = jnp.minimum(tallies[donor] - 1, reach - tallies[taker]) // 2
    slack = jnp.where((donor == ranking[0]) | (taker == ranking[0]) | (tallies[taker] == 0), 0, jnp.maximum(slack, 0))
    passed = jax.random.randint(jax.random.fold_in(own, 4), (count // 2,), 0, 1 << 20) % (slack + 1)
    tallies = tallies.at[donor].add(-passed).at[taker].add(passed)
    members = jnp.searchsorted(jnp.cumsum(tallies), jnp.arange(rows * top), side="right").astype(jnp.int32)
    listing = members.reshape(top, rows).T
    listing = listing[jax.random.permutation(jax.random.fold_in(own, 1), rows)]
    rotation = jax.random.randint(jax.random.fold_in(own, 2), (rows, 1), 0, top)
    return jnp.take_along_axis(listing, (jnp.arange(top)[None, :] + rotation) % top, axis=1)


def portions_of(amount, total, bound, lean, full):
    portions = [(1 << 20) // math.isqrt(rank ** lean) + 1 for rank in range(1, amount + 1)]
    largest = bound if full else min(bound, max(-(-total // amount), total * portions[0] // sum(portions)))
    least = 1 if total - largest >= amount - 1 else 0
    given, surplus = [largest] + [least] * (amount - 1), total - largest - least * (amount - 1)
    while surplus > 0:
        candidates = [i for i in range(1, amount) if given[i] < largest] or [i for i in range(1, amount) if given[i] < bound]
        pool, remaining = sum([portions[i] for i in candidates]), surplus
        for i in candidates:
            more = min(bound - given[i], max(1, remaining * portions[i] // pool), surplus)
            given[i] = given[i] + more
            surplus = surplus - more
    return np.array(given)


def bell_draw(key, shape, spread, most, split=(), held_as=jnp.bfloat16):
    array = jax.random.normal(key, shape, jnp.float32) * spread
    if len(split) > 0:
        array = block_levels(key, shape, split, -0.22, 0.18) * array
    return jnp.clip(array, min=-most, max=most).astype(held_as)


def setup_inputs(seed: int = 0) -> dict:
    key_list = jax.random.split(jax.random.key(seed), 8)
    tokens = bell_draw(key_list[0], (TOKENS, D), 1.0, 6.0, ((0, 16),))
    norm_gain = jnp.clip(1.0 + 0.18 * jax.random.normal(key_list[1], (D,), jnp.float32), 0.1, 1.9)
    routing_keys = jax.random.split(jax.random.fold_in(key_list[2], 1), TOKENS // TOK_DEV)
    routing_turns = jax.random.permutation(jax.random.fold_in(key_list[2], 3), TOKENS // TOK_DEV)
    routing = jax.vmap(lambda own, number: routed_block(jax.random.fold_in(key_list[2], 2), own, number, TOK_DEV, EXPERTS, TOPK, CAP, 2))(routing_keys, routing_turns).reshape((TOKENS, TOPK))
    route_logits = bell_draw(key_list[3], (TOKENS, TOPK), 1.5, 6.0, ((0, 16),), jnp.float32)
    w_gate = bell_draw(key_list[4], (EXPERTS, D, FF), D ** -0.5, 0.1875, ((0, 16), (2, 2)))
    w_up = bell_draw(key_list[5], (EXPERTS, D, FF), D ** -0.5, 0.1875, ((0, 16), (2, 2)))
    w_down = bell_draw(key_list[6], (EXPERTS, FF, D), FF ** -0.5, 0.1875, ((0, 16), (2, 2)))
    return dict(tokens=tokens, norm_gain=norm_gain, routing=routing, route_logits=route_logits, w_gate=w_gate, w_up=w_up, w_down=w_down)


eps = 1e-5


def clamped(gate_part, up_part):
    limited = jnp.minimum(gate_part, 7.0)
    linear = jnp.clip(up_part, -7.0, 7.0)
    return limited * jax.nn.sigmoid(1.702 * limited) * (linear + 1.0)


def reference(tokens, norm_gain, routing, route_logits, w_gate, w_up, w_down):
    as_float = tokens.astype(jnp.float32)
    scaled = as_float * lax.rsqrt(jnp.mean(as_float * as_float, axis=-1, keepdims=True) + eps)
    normed = (scaled * norm_gain).astype(jnp.bfloat16)
    probs = jax.nn.softmax(route_logits, axis=-1)
    count_tok = routing.shape[0]
    topk = routing.shape[1]
    assigns = count_tok * topk
    block_rows = 32
    flat_e = routing.reshape(-1).astype(jnp.int32)
    flat_tok = (jnp.arange(assigns, dtype=jnp.int32) // topk).astype(jnp.int32)
    flat_w = probs.reshape(-1)
    order = jnp.argsort(flat_e, stable=True).astype(jnp.int32)
    sorted_e = flat_e[order]
    counts = jnp.bincount(flat_e, length=EXPERTS).astype(jnp.int32)
    starts = (jnp.cumsum(counts) - counts).astype(jnp.int32)
    padded = ((counts + block_rows - 1) // block_rows * block_rows).astype(jnp.int32)
    pends = jnp.cumsum(padded).astype(jnp.int32)
    pstarts = (pends - padded).astype(jnp.int32)
    dest = (pstarts[sorted_e] + jnp.arange(assigns, dtype=jnp.int32) - starts[sorted_e]).astype(jnp.int32)
    n_blocks = -(-assigns // block_rows) + EXPERTS
    n_rows = n_blocks * block_rows
    row_tok = jnp.full((n_rows,), count_tok, dtype=jnp.int32).at[dest].set(flat_tok[order])
    row_w = jnp.zeros((n_rows,), jnp.float32).at[dest].set(flat_w[order])
    block_e = jnp.minimum(
        jnp.searchsorted(pends, jnp.arange(n_blocks, dtype=jnp.int32) * block_rows, side="right").astype(jnp.int32),
        EXPERTS - 1).astype(jnp.int32)
    x_pad = jnp.concatenate([normed, jnp.zeros((1, normed.shape[1]), jnp.bfloat16)], axis=0)
    blocks_in = x_pad[row_tok].reshape(n_blocks, block_rows, normed.shape[1])

    def expert_block(pair):
        rows, expert = pair
        gate_part = jnp.dot(rows, w_gate[expert], preferred_element_type=jnp.float32)
        up_part = jnp.dot(rows, w_up[expert], preferred_element_type=jnp.float32)
        hidden = clamped(gate_part, up_part).astype(jnp.bfloat16)
        return jnp.dot(hidden, w_down[expert], preferred_element_type=jnp.float32).astype(jnp.bfloat16)

    outs_rows = lax.map(expert_block, (blocks_in, block_e)).reshape(n_rows, normed.shape[1])
    summed = jax.ops.segment_sum(outs_rows.astype(jnp.float32) * row_w[:, None], row_tok, num_segments=count_tok + 1)
    return summed[:count_tok].astype(jnp.bfloat16)
```

```python
import functools

import jax
import jax.numpy as jnp
from jax import lax
from jax.experimental import pallas as pl
from jax.experimental.pallas import tpu as pltpu
from jax.sharding import PartitionSpec as P

CAP = 16
MESH = pl.DeviceIdType.MESH

eps = 1e-05


def each(count, step):
    if count <= 16:
        for k in range(count):
            step(k)
    else:
        lax.fori_loop(0, count, lambda k, carry: (step(k), carry)[1], 0)


def mm(a, b):
    return jnp.dot(a, b, preferred_element_type=jnp.float32)


def kernel(n, x_ref, gain_ref, route_ref, logit_ref, wg_hbm, wu_hbm, wd_hbm, out_ref,
           wg, wu, wd, outb, arr, gp, up, hid, eo, ret,
           wsem, dsend, drecv, fsend, frecv, hsend, hrecv, rsend, rrecv):
    me, c = lax.axis_index("ep"), lax.axis_index("tp")
    other = 1 - c
    tok, width = x_ref.shape
    topk = route_ref.shape[1]
    half = outb.shape[2]
    fh = hid.shape[2]
    dh = eo.shape[2]
    rows = n * CAP
    step_rows = min(rows, 256)

    barrier = pltpu.get_barrier_semaphore()
    pl.semaphore_signal(barrier, inc=1, device_id=(me, other), device_id_type=MESH)

    def greet(k):
        pl.semaphore_signal(barrier, inc=1, device_id=(lax.rem(me + k + 1, n), c), device_id_type=MESH)

    each(n - 1, greet)

    loads = [pltpu.make_async_copy(src.at[0], dst, wsem.at[i])
             for i, (src, dst) in enumerate(((wg_hbm, wg), (wu_hbm, wu), (wd_hbm, wd)))]
    for load in loads:
        load.start()

    lane = lax.broadcasted_iota(jnp.int32, (tok, rows), 1)
    expert, slot = lax.div(lane, CAP), lax.rem(lane, CAP)
    route = route_ref[...]
    logits = logit_ref[...]
    raised = jnp.exp(logits - jnp.max(logits, axis=1, keepdims=True))
    probs = raised / jnp.sum(raised, axis=1, keepdims=True)
    named = jnp.zeros((tok, rows), jnp.float32)
    weight = jnp.zeros((tok, rows), jnp.float32)
    for k in range(topk):
        hit = route[:, k:k + 1] == expert
        named = jnp.where(hit, 1.0, named)
        weight = jnp.where(hit, probs[:, k:k + 1], weight)
    earlier = (lax.broadcasted_iota(jnp.int32, (tok, tok), 1)
               < lax.broadcasted_iota(jnp.int32, (tok, tok), 0))
    earlier = jnp.where(earlier, 1.0, 0.0).astype(jnp.bfloat16)
    rank = mm(earlier, named.astype(jnp.bfloat16))
    here = rank == slot.astype(jnp.float32)
    place = jnp.where(here, named, 0.0).astype(jnp.bfloat16)
    weight = jnp.where(here, weight, 0.0)

    x = x_ref[...].astype(jnp.float32)
    inv = lax.rsqrt(jnp.mean(x * x, axis=1, keepdims=True) + eps)
    own_cols = pl.ds(pl.multiple_of(c * half, half), half)
    mine = ((x_ref[:, own_cols].astype(jnp.float32) * inv) * gain_ref[:, own_cols]).astype(jnp.bfloat16)
    outb[...] = lax.dot_general(place, mine, (((0,), (0,)), ((), ())),
                                preferred_element_type=jnp.float32).astype(jnp.bfloat16).reshape(n, CAP, half)
    arr[c, me] = outb[me]

    pl.semaphore_wait(barrier, n)

    def forward(source):
        pltpu.make_async_remote_copy(
            arr.at[c, source], arr.at[c, source], fsend, frecv,
            device_id=(me, other), device_id_type=MESH).start()

    def send(k):
        to = lax.rem(me + k + 1, n)
        pltpu.make_async_remote_copy(
            outb.at[to], arr.at[c, me], dsend, drecv.at[me],
            device_id=(to, c), device_id_type=MESH).start()

    each(n - 1, send)
    forward(me)

    def pass_on(k):
        source = lax.rem(me + n - k - 1, n)
        pltpu.make_async_remote_copy(
            outb.at[source], arr.at[c, source], dsend, drecv.at[source],
            device_id=(source, c), device_id_type=MESH).wait_recv()
        forward(source)

    each(n - 1, pass_on)

    own_in = pl.ds(pl.multiple_of(c * half, half), half)
    other_in = pl.ds(pl.multiple_of(other * half, half), half)
    own_hid = pl.ds(pl.multiple_of(c * fh, fh), fh)
    other_hid = pl.ds(pl.multiple_of(other * fh, fh), fh)
    per = step_rows // CAP
    loads[0].wait()
    loads[1].wait()

    def first_half(i):
        rs = pl.ds(i * step_rows, step_rows)
        a = arr[c, pl.ds(i * per, per)].reshape(step_rows, half)
        gp[rs] = mm(a, wg[own_in])
        up[rs] = mm(a, wu[own_in])

    each(rows // step_rows, first_half)
    pltpu.make_async_copy(arr.at[other], arr.at[other], frecv).wait()

    def second_half(i):
        rs = pl.ds(i * step_rows, step_rows)
        a = arr[other, pl.ds(i * per, per)].reshape(step_rows, half)
        g = jnp.minimum(gp[rs] + mm(a, wg[other_in]), 7.0)
        l = jnp.clip(up[rs] + mm(a, wu[other_in]), -7.0, 7.0)
        hid[c, rs] = (g * jax.nn.sigmoid(1.702 * g) * (l + 1.0)).astype(jnp.bfloat16)

    each(rows // step_rows, second_half)
    swap = pltpu.make_async_remote_copy(
        hid.at[c], hid.at[c], hsend, hrecv, device_id=(me, other), device_id_type=MESH)
    swap.start()
    loads[2].wait()

    def first_down(i):
        rs = pl.ds(i * step_rows, step_rows)
        gp[rs] = mm(hid[c, rs], wd[own_hid])

    each(rows // step_rows, first_down)
    pltpu.make_async_copy(hid.at[other], hid.at[other], hrecv).wait()

    def second_down(i):
        rs = pl.ds(i * step_rows, step_rows)
        total = gp[rs] + mm(hid[other, rs], wd[other_hid])
        eo[pl.ds(i * per, per)] = total.astype(jnp.bfloat16).reshape(per, CAP, dh)

    each(rows // step_rows, second_down)

    def give_back(k):
        to = lax.rem(me + k + 1, n)
        pltpu.make_async_remote_copy(
            eo.at[to], ret.at[me], rsend, rrecv,
            device_id=(to, c), device_id_type=MESH).start()

    each(n - 1, give_back)
    ret[me] = eo[me]
    high = weight.astype(jnp.bfloat16)
    low = (weight - high.astype(jnp.float32)).astype(jnp.bfloat16)
    others = pl.ds(0, n - 1)
    pltpu.make_async_copy(ret.at[others], ret.at[others], rrecv).wait()
    back = ret[...].reshape(rows, dh)
    out_ref[...] = (mm(high, back) + mm(low, back)).astype(out_ref.dtype)

    pltpu.make_async_copy(outb.at[others], outb.at[others], dsend).wait()
    pltpu.make_async_copy(arr.at[c], arr.at[c], fsend).wait()
    swap.wait_send()
    pltpu.make_async_copy(eo.at[others], eo.at[others], rsend).wait()


def shards(tokens, norm_gain, routing, route_logits, w_gate, w_up, w_down):
    n = lax.axis_size("ep")
    tok, width = tokens.shape
    half = width // lax.axis_size("tp")
    fh = w_gate.shape[2]
    dh = w_down.shape[2]
    rows = n * CAP
    vmem = pl.BlockSpec(memory_space=pltpu.VMEM)
    hbm = pl.BlockSpec(memory_space=pl.ANY)
    bf16, f32 = jnp.bfloat16, jnp.float32
    dma = pltpu.SemaphoreType.DMA
    return pl.pallas_call(
        functools.partial(kernel, n),
        out_shape=jax.ShapeDtypeStruct((tok, dh), bf16),
        in_specs=[vmem] * 4 + [hbm] * 3,
        out_specs=vmem,
        scratch_shapes=[
            pltpu.VMEM(w_gate.shape[1:], bf16),
            pltpu.VMEM(w_up.shape[1:], bf16),
            pltpu.VMEM(w_down.shape[1:], bf16),
            pltpu.VMEM((n, CAP, half), bf16),
            pltpu.VMEM((2, n, CAP, half), bf16),
            pltpu.VMEM((rows, fh), f32),
            pltpu.VMEM((rows, fh), f32),
            pltpu.VMEM((2, rows, fh), bf16),
            pltpu.VMEM((n, CAP, dh), bf16),
            pltpu.VMEM((n, CAP, dh), bf16),
            dma((3,)),
            dma,
            dma((n,)),
            dma,
            dma,
            dma,
            dma,
            dma,
            dma,
        ],
        compiler_params=pltpu.CompilerParams(
            collective_id=0, has_side_effects=True, vmem_limit_bytes=60 * 1024 * 1024),
    )(tokens, norm_gain.reshape(1, width), routing, route_logits, w_gate, w_up, w_down)


def solution(mesh):
    return jax.shard_map(
        shards,
        mesh=mesh,
        in_specs=(
            P("ep", None),
            P(),
            P("ep", None),
            P("ep", None),
            P("ep", None, "tp"),
            P("ep", None, "tp"),
            P("ep", None, "tp"),
        ),
        out_specs=P("ep", "tp"),
        check_vma=False,
    )
```

```python
import functools

import jax
import jax.numpy as jnp
from jax import lax
from jax.experimental import pallas as pl
from jax.experimental.pallas import tpu as pltpu
from jax.sharding import PartitionSpec as P

CAP = 16
MESH = pl.DeviceIdType.MESH

eps = 1e-05


def each(count, step):
    if count <= 16:
        for k in range(count):
            step(k)
    else:
        lax.fori_loop(0, count, lambda k, carry: (step(k), carry)[1], 0)


def mm(a, b):
    return jnp.dot(a, b, preferred_element_type=jnp.float32)


def kernel(n, x_ref, gain_ref, route_ref, logit_ref, wg_hbm, wu_hbm, wd_hbm, out_ref,
           wg, wu, wd, outb, arr, gp, up, hid, eo, ret,
           wsem, dsend, drecv, fsend, frecv, hsend, hrecv, rsend, rrecv):
    me, c = lax.axis_index("ep"), lax.axis_index("tp")
    other = 1 - c
    tok, width = x_ref.shape
    topk = route_ref.shape[1]
    half = outb.shape[2]
    fh = hid.shape[2]
    dh = eo.shape[2]
    rows = n * CAP
    step_rows = min(rows // 2, 256)

    barrier = pltpu.get_barrier_semaphore()
    pl.semaphore_signal(barrier, inc=1, device_id=(me, other), device_id_type=MESH)

    def greet(k):
        pl.semaphore_signal(barrier, inc=1, device_id=(lax.rem(me + k + 1, n), c), device_id_type=MESH)

    each(n - 1, greet)

    loads = [pltpu.make_async_copy(src.at[0], dst, wsem.at[i])
             for i, (src, dst) in enumerate(((wg_hbm, wg), (wu_hbm, wu), (wd_hbm, wd)))]
    for load in loads:
        load.start()

    lane = lax.broadcasted_iota(jnp.int32, (tok, rows), 1)
    expert, slot = lax.div(lane, CAP), lax.rem(lane, CAP)
    route = route_ref[...]
    logits = logit_ref[...]
    raised = jnp.exp(logits - jnp.max(logits, axis=1, keepdims=True))
    probs = raised / jnp.sum(raised, axis=1, keepdims=True)
    named = jnp.zeros((tok, rows), jnp.float32)
    weight = jnp.zeros((tok, rows), jnp.float32)
    for k in range(topk):
        hit = route[:, k:k + 1] == expert
        named = jnp.where(hit, 1.0, named)
        weight = jnp.where(hit, probs[:, k:k + 1], weight)
    earlier = (lax.broadcasted_iota(jnp.int32, (tok, tok), 1)
               < lax.broadcasted_iota(jnp.int32, (tok, tok), 0))
    earlier = jnp.where(earlier, 1.0, 0.0).astype(jnp.bfloat16)
    rank = mm(earlier, named.astype(jnp.bfloat16))
    here = rank == slot.astype(jnp.float32)
    place = jnp.where(here, named, 0.0).astype(jnp.bfloat16)
    weight = jnp.where(here, weight, 0.0)

    x = x_ref[...].astype(jnp.float32)
    inv = lax.rsqrt(jnp.mean(x * x, axis=1, keepdims=True) + eps)
    own_cols = pl.ds(pl.multiple_of(c * half, half), half)
    mine = ((x_ref[:, own_cols].astype(jnp.float32) * inv) * gain_ref[:, own_cols]).astype(jnp.bfloat16)
    outb[...] = lax.dot_general(place, mine, (((0,), (0,)), ((), ())),
                                preferred_element_type=jnp.float32).astype(jnp.bfloat16).reshape(n, CAP, half)
    arr[c, me] = outb[me]

    pl.semaphore_wait(barrier, n)

    group = n // 2
    own_base = lax.div(me, group) * group
    far_base = (n - group) - own_base
    at = me - own_base

    def forward(source, part):
        pltpu.make_async_remote_copy(
            arr.at[c, source], arr.at[c, source], fsend, frecv.at[part],
            device_id=(me, other), device_id_type=MESH).start()

    def near(k):
        return own_base + lax.rem(at + k + 1, group)

    def far(k):
        return far_base + lax.rem(at + k, group)

    def send(to):
        pltpu.make_async_remote_copy(
            outb.at[to], arr.at[c, me], dsend, drecv.at[me],
            device_id=(to, c), device_id_type=MESH).start()

    def pass_on(source, part):
        pltpu.make_async_remote_copy(
            outb.at[source], arr.at[c, source], dsend, drecv.at[source],
            device_id=(source, c), device_id_type=MESH).wait_recv()
        forward(source, part)

    def give_back(to):
        pltpu.make_async_remote_copy(
            eo.at[to], ret.at[me], rsend, rrecv,
            device_id=(to, c), device_id_type=MESH).start()

    each(group, lambda k: send(far(k)))
    each(group - 1, lambda k: send(near(k)))
    forward(me, 0)

    own_in = pl.ds(pl.multiple_of(c * half, half), half)
    other_in = pl.ds(pl.multiple_of(other * half, half), half)
    own_hid = pl.ds(pl.multiple_of(c * fh, fh), fh)
    other_hid = pl.ds(pl.multiple_of(other * fh, fh), fh)
    per = step_rows // CAP
    steps = group * CAP // step_rows

    def run_experts(part, base):
        whole = pl.ds(base, group)
        first_row = pl.multiple_of(base * CAP, group * CAP)
        whole_rows = pl.ds(first_row, group * CAP)

        def rows_at(i):
            return pl.ds(pl.multiple_of(first_row + i * step_rows, step_rows), step_rows)

        def blocks_at(i):
            return pl.ds(base + i * per, per)

        def first_half(i):
            rs = rows_at(i)
            a = arr[c, blocks_at(i)].reshape(step_rows, half)
            gp[rs] = mm(a, wg[own_in])
            up[rs] = mm(a, wu[own_in])

        each(steps, first_half)
        waited = arr.at[other, whole]
        pltpu.make_async_copy(waited, waited, frecv.at[part]).wait()

        def second_half(i):
            rs = rows_at(i)
            a = arr[other, blocks_at(i)].reshape(step_rows, half)
            g = jnp.minimum(gp[rs] + mm(a, wg[other_in]), 7.0)
            l = jnp.clip(up[rs] + mm(a, wu[other_in]), -7.0, 7.0)
            hid[c, rs] = (g * jax.nn.sigmoid(1.702 * g) * (l + 1.0)).astype(jnp.bfloat16)

        each(steps, second_half)
        swap = pltpu.make_async_remote_copy(
            hid.at[c, whole_rows], hid.at[c, whole_rows], hsend.at[part], hrecv.at[part],
            device_id=(me, other), device_id_type=MESH)
        swap.start()
        if part == 0:
            loads[2].wait()

        def first_down(i):
            rs = rows_at(i)
            gp[rs] = mm(hid[c, rs], wd[own_hid])

        each(steps, first_down)
        swapped = hid.at[other, whole_rows]
        pltpu.make_async_copy(swapped, swapped, hrecv.at[part]).wait()

        def second_down(i):
            rs = rows_at(i)
            total = gp[rs] + mm(hid[other, rs], wd[other_hid])
            eo[blocks_at(i)] = total.astype(jnp.bfloat16).reshape(per, CAP, dh)

        each(steps, second_down)
        return swap

    each(group - 1, lambda k: pass_on(near(group - 2 - k), 0))
    loads[0].wait()
    loads[1].wait()
    swap_near = run_experts(0, own_base)
    each(group - 1, lambda k: give_back(near(k)))
    each(group, lambda k: pass_on(far(k), 1))
    swap_far = run_experts(1, far_base)
    each(group, lambda k: give_back(far(k)))
    ret[me] = eo[me]
    high = weight.astype(jnp.bfloat16)
    low = (weight - high.astype(jnp.float32)).astype(jnp.bfloat16)
    others = pl.ds(0, n - 1)
    pltpu.make_async_copy(ret.at[others], ret.at[others], rrecv).wait()
    back = ret[...].reshape(rows, dh)
    out_ref[...] = (mm(high, back) + mm(low, back)).astype(out_ref.dtype)

    pltpu.make_async_copy(outb.at[others], outb.at[others], dsend).wait()
    pltpu.make_async_copy(arr.at[c], arr.at[c], fsend).wait()
    swap_near.wait_send()
    swap_far.wait_send()
    pltpu.make_async_copy(eo.at[others], eo.at[others], rsend).wait()


def shards(tokens, norm_gain, routing, route_logits, w_gate, w_up, w_down):
    n = lax.axis_size("ep")
    tok, width = tokens.shape
    half = width // lax.axis_size("tp")
    fh = w_gate.shape[2]
    dh = w_down.shape[2]
    rows = n * CAP
    vmem = pl.BlockSpec(memory_space=pltpu.VMEM)
    hbm = pl.BlockSpec(memory_space=pl.ANY)
    bf16, f32 = jnp.bfloat16, jnp.float32
    dma = pltpu.SemaphoreType.DMA
    return pl.pallas_call(
        functools.partial(kernel, n),
        out_shape=jax.ShapeDtypeStruct((tok, dh), bf16),
        in_specs=[vmem] * 4 + [hbm] * 3,
        out_specs=vmem,
        scratch_shapes=[
            pltpu.VMEM(w_gate.shape[1:], bf16),
            pltpu.VMEM(w_up.shape[1:], bf16),
            pltpu.VMEM(w_down.shape[1:], bf16),
            pltpu.VMEM((n, CAP, half), bf16),
            pltpu.VMEM((2, n, CAP, half), bf16),
            pltpu.VMEM((rows, fh), f32),
            pltpu.VMEM((rows, fh), f32),
            pltpu.VMEM((2, rows, fh), bf16),
            pltpu.VMEM((n, CAP, dh), bf16),
            pltpu.VMEM((n, CAP, dh), bf16),
            dma((3,)),
            dma,
            dma((n,)),
            dma,
            dma((2,)),
            dma((2,)),
            dma((2,)),
            dma,
            dma,
        ],
        compiler_params=pltpu.CompilerParams(
            collective_id=0, has_side_effects=True, vmem_limit_bytes=60 * 1024 * 1024),
    )(tokens, norm_gain.reshape(1, width), routing, route_logits, w_gate, w_up, w_down)


def solution(mesh):
    return jax.shard_map(
        shards,
        mesh=mesh,
        in_specs=(
            P("ep", None),
            P(),
            P("ep", None),
            P("ep", None),
            P("ep", None, "tp"),
            P("ep", None, "tp"),
            P("ep", None, "tp"),
        ),
        out_specs=P("ep", "tp"),
        check_vma=False,
    )
```
